32 devices in a mesh: sp: 4 (over z), fs: 4 (over y, x), tp: 2 (over core).
Axes of the slice: x: 2, y: 2, z: 4, core: 2. Of those that a mesh axis runs over, the one named last changes fastest.
Arguments:
- tokens: bfloat16 [4, 2048, 2048], P('fs', 'sp', 'tp'), may hold values from -6 to 6
- norm_gain: float32 [2048], replicated, may hold values from 0.1 to 1.9
- query_weight: bfloat16 [2048, 1024], P(('sp', 'fs'), 'tp'), may hold values from -0.125 to 0.125
- key_weight: bfloat16 [2048, 1024], P(('sp', 'fs'), 'tp'), may hold values from -0.125 to 0.125
- value_weight: bfloat16 [2048, 2048], P(('sp', 'fs'), 'tp'), may hold values from -0.125 to 0.125
- outgate_weight: bfloat16 [2048, 2048], P(('sp', 'fs'), 'tp'), may hold values from -0.125 to 0.125
- gate_weight: bfloat16 [2048, 2, 16], P(('sp', 'fs'), None, 'tp'), may hold values from -6 to 6
- forget_bias: float32 [16], P('tp')
- forget_shift: float32 [4, 16, 2048], P('fs', 'tp', 'sp'), may hold values from -1.5 to 0
- head_norm_gain: float32 [2048], P('tp'), may hold values from 0.1 to 1.9
- exit_weight: bfloat16 [2048, 2048], P(('sp', 'fs'), 'tp'), may hold values from -0.125 to 0.125
- entry_weight: bfloat16 [2048, 2048], P(('sp', 'fs'), 'tp'), may hold values from -0.125 to 0.125
- signal_weight: bfloat16 [2048, 2048], P(('sp', 'fs'), 'tp'), may hold values from -0.125 to 0.125
- conv_kernel: float32 [3, 2048], P(None, 'tp'), may hold values from -3.5 to 3.5
- merge_weight: bfloat16 [4096, 2048], P(('sp', 'fs'), 'tp'), may hold values from -0.09375 to 0.09375
Outputs:
- mixed: bfloat16 [4, 2048, 2048], P('fs', 'sp', 'tp')
The draws below stay inside these ranges and needn't reach their ends.
All inputs are finite; a program needn't handle non-finite values.
Results may differ from the reference program's by a relative error of at most 0.017.
The reference program's roundings to bfloat16 on the way count: a program that leaves them out, or rounds other values in their place, can miss the bound.
Values may be sent and summed in bfloat16 or wider, within the bound.
A program may use at most 128 MiB of HBM per device.

```python
import math
import jax
import jax.numpy as jnp
from jax import lax

D = 2048
HEADS = 16
DK = 64
DV = 128
CONV = 2048
BLOCK = 128
KERNEL = 3
TOK_DEV = 512
LEN = 2048
SEQS = 4


def draw_gate_weight(key, part):
    base = jax.random.normal(key, (D, 2, HEADS), jnp.float32) * D ** (-0.5)
    return jnp.clip(base, -6.0, 6.0).astype(jnp.bfloat16)


def draw_forget_bias(key, part):
    pick_key, quick_key, steady_key = jax.random.split(key, 3)
    share = 0.5
    fast = jax.random.uniform(pick_key, (HEADS,), jnp.float32) < share
    quick = jax.random.uniform(quick_key, (HEADS,), jnp.float32, 2.5, 4.0)
    constant_quantity = math.log(LEN) + jax.random.uniform(steady_key, (HEADS,), jnp.float32, 1.5, 2.5)
    return jnp.where(fast, quick, constant_quantity).astype(jnp.float32)


def draw_forget_shift(key, part):
    rate_key, place_key, depth_key = jax.random.split(key, 3)
    segments = LEN // TOK_DEV
    rates = jnp.exp(jax.random.uniform(rate_key, (SEQS, HEADS, segments), jnp.float32, math.log(0.05), 0.0)) / LEN
    constant_quantity = -jnp.repeat(rates, TOK_DEV, axis=2)
    places = jax.random.randint(place_key, (SEQS, HEADS, 2), 0, LEN)
    layer_tiers = jax.random.uniform(depth_key, (SEQS, HEADS, 2), jnp.float32, 0.22, 0.69)
    positions = jnp.arange(LEN, dtype=jnp.int32)
    agreement_tally = (positions[None, None, None, :] == places[..., None]).astype(jnp.float32)
    spike_clusters = -jnp.sum(agreement_tally * layer_tiers[..., None], axis=2)
    return (constant_quantity + spike_clusters).astype(jnp.float32)


def block_scale(rng, dims, shards, smallest, top_value):
    loudness, own = 1.0, jax.random.fold_in(rng, 6)
    for position, blocks in shards:
        steps = jnp.exp(jax.random.uniform(jax.random.fold_in(own, position), (blocks,), jnp.float32, smallest / len(shards), top_value / len(shards)))
        loudness = loudness * jnp.repeat(steps, dims[position] // blocks).reshape([-1 if axis == position else 1 for axis in range(len(dims))])
    return loudness


def centred(stream_key, dims, scale, limit, cuts=(), kind=jnp.bfloat16):
    result = scale * jax.random.normal(stream_key, dims, jnp.float32)
    if cuts:
        result = result * block_scale(stream_key, dims, cuts, -0.22, 0.18)
    return jnp.clip(result, -limit, limit).astype(kind)


def setup_inputs(seed: int = 0) -> dict:
    arg_keys = jax.random.split(jax.random.key(seed), 16)
    tokens = centred(arg_keys[0], (SEQS, LEN, D), 1.0, 6.0, ((0, 4), (1, 4), (2, 2)))
    norm_gain = jnp.clip(1.0 + 0.18 * jax.random.normal(arg_keys[1], (D,), jnp.float32), 0.1, 1.9)
    query_weight = centred(arg_keys[2], (D, HEADS * DK), D ** -0.5, 0.125, ((0, 16), (1, 2)))
    key_weight = centred(arg_keys[3], (D, HEADS * DK), D ** -0.5, 0.125, ((0, 16), (1, 2)))
    value_weight = centred(arg_keys[4], (D, HEADS * DV), D ** -0.5, 0.125, ((0, 16), (1, 2)))
    outgate_weight = centred(arg_keys[5], (D, HEADS * DV), D ** -0.5, 0.125, ((0, 16), (1, 2)))
    gate_weight = draw_gate_weight(jax.random.fold_in(arg_keys[15], 71), 0)
    forget_bias = draw_forget_bias(jax.random.fold_in(arg_keys[15], 71), 0)
    forget_shift = draw_forget_shift(jax.random.fold_in(arg_keys[15], 71), 0)
    head_norm_gain = jnp.clip(1.0 + 0.18 * jax.random.normal(arg_keys[9], (HEADS * DV,), jnp.float32), 0.1, 1.9)
    exit_weight = centred(arg_keys[10], (D, CONV), D ** -0.5, 0.125, ((0, 16), (1, 2)))
    entry_weight = centred(arg_keys[11], (D, CONV), D ** -0.5, 0.125, ((0, 16), (1, 2)))
    signal_weight = centred(arg_keys[12], (D, CONV), D ** -0.5, 0.125, ((0, 16), (1, 2)))
    conv_kernel = centred(arg_keys[13], (KERNEL, CONV), KERNEL ** -0.5, 3.5, ((1, 2),), jnp.float32)
    merge_weight = centred(arg_keys[14], (HEADS * DV + CONV, D), (HEADS * DV + CONV) ** -0.5, 0.09375, ((0, 16), (1, 2)))
    return {"tokens": tokens, "norm_gain": norm_gain, "query_weight": query_weight, "key_weight": key_weight, "value_weight": value_weight, "outgate_weight": outgate_weight, "gate_weight": gate_weight, "forget_bias": forget_bias, "forget_shift": forget_shift, "head_norm_gain": head_norm_gain, "exit_weight": exit_weight, "entry_weight": entry_weight, "signal_weight": signal_weight, "conv_kernel": conv_kernel, "merge_weight": merge_weight}


EPSILON = 1e-06
HIGHEST = lax.Precision.HIGHEST

def reference(tokens, norm_gain, query_weight, key_weight, value_weight, outgate_weight, gate_weight, forget_bias, forget_shift, head_norm_gain, exit_weight, entry_weight, signal_weight, conv_kernel, merge_weight):
    count = SEQS * LEN
    blocks = LEN // BLOCK
    flat = tokens.astype(jnp.float32)
    normed = (flat * lax.rsqrt(lax.optimization_barrier(jnp.mean(flat * flat, axis=-1, keepdims=True)) + EPSILON) * norm_gain).astype(jnp.bfloat16)
    rows = normed.reshape(count, D)

    def project(weight):
        return jnp.dot(rows, weight, preferred_element_type=jnp.float32)
    queries = project(query_weight).astype(jnp.bfloat16)
    keys = project(key_weight).astype(jnp.bfloat16)
    values = project(value_weight).astype(jnp.bfloat16)
    outgates = project(outgate_weight).astype(jnp.bfloat16)
    exit_rows = project(exit_weight).astype(jnp.bfloat16)
    entry_rows = project(entry_weight).astype(jnp.bfloat16)
    signal_rows = project(signal_weight).astype(jnp.bfloat16)
    gates = project(gate_weight.reshape(D, 2 * HEADS))

    def split_heads(array, width):
        return array.reshape(SEQS, blocks, BLOCK, HEADS, width).transpose(0, 3, 1, 2, 4).astype(jnp.float32)

    def lanes(array):
        return array.reshape(SEQS, blocks, BLOCK, HEADS).transpose(0, 3, 1, 2)
    inputs = lanes(gates[:, :HEADS])
    logs = lanes(jax.nn.log_sigmoid(gates[:, HEADS:] + forget_bias)) + forget_shift.reshape(SEQS, HEADS, blocks, BLOCK)
    query_float = split_heads(queries, DK)
    key_float = split_heads(keys, DK)
    value_float = split_heads(values, DV)
    scale = DK ** (-0.5)
    cumulative = jnp.cumsum(logs, axis=-1)
    last = cumulative[..., -1]
    weight_logs = last[..., None] - cumulative + inputs
    peak = lax.optimization_barrier(jnp.max(weight_logs, axis=-1))
    coefficient_array = jnp.exp(weight_logs - peak[..., None])
    scaled = key_float * scale
    states = jnp.einsum('bhcs,bhcsk,bhcsv->bhckv', coefficient_array, scaled, value_float, precision=HIGHEST)

    def step(carry, item):
        state, bounded_maximum = carry
        block_last, block_peak, block_state = item
        ceiling = jnp.maximum(block_last + bounded_maximum, block_peak)
        kept = jnp.exp(block_last + bounded_maximum - ceiling)
        added = jnp.exp(block_peak - ceiling)
        new_state = kept[..., None, None] * state + added[..., None, None] * block_state
        return ((new_state, ceiling), (state, bounded_maximum))
    start = (jnp.zeros((SEQS, HEADS, DK, DV), jnp.float32), jnp.zeros((SEQS, HEADS), jnp.float32))
    items = (jnp.moveaxis(last, 2, 0), jnp.moveaxis(peak, 2, 0), jnp.moveaxis(states, 2, 0))
    unused, before = lax.scan(step, start, items)
    state_prev = jnp.moveaxis(before[0], 0, 2)
    stable_prev = jnp.moveaxis(before[1], 0, 2)
    score_matrix = jnp.einsum('bhcjk,bhcsk->bhcjs', query_float, key_float) * scale
    causal = jnp.tril(jnp.ones((BLOCK, BLOCK), dtype=bool))
    decay = jnp.where(causal, cumulative[..., :, None] - cumulative[..., None, :] + inputs[..., None, :], -jnp.inf)
    inter = cumulative + stable_prev[..., None]
    ceiling = jnp.maximum(inter, lax.optimization_barrier(jnp.max(decay, axis=-1)))
    weighted = score_matrix * jnp.exp(decay - ceiling[..., None])
    rounded = lax.optimization_barrier(weighted.astype(jnp.bfloat16)).astype(jnp.float32)
    carried = jnp.exp(inter - ceiling)
    numerator = jnp.einsum('bhcjs,bhcsv->bhcjv', rounded, value_float)
    numerator = numerator + carried[..., None] * jnp.einsum('bhcjk,bhckv->bhcjv', query_float, state_prev, precision=HIGHEST)
    hidden = numerator * lax.rsqrt(lax.optimization_barrier(jnp.mean(numerator * numerator, axis=-1, keepdims=True)) + EPSILON)
    hidden = hidden.transpose(0, 2, 3, 1, 4).reshape(count, HEADS * DV) * head_norm_gain
    memory_out = (hidden * jax.nn.sigmoid(outgates.astype(jnp.float32))).astype(jnp.bfloat16)
    mixed_in = (entry_rows.astype(jnp.float32) * signal_rows.astype(jnp.float32)).astype(jnp.bfloat16)
    padded = jnp.pad(mixed_in.reshape(SEQS, LEN, CONV).astype(jnp.float32), ((0, 0), (KERNEL - 1, 0), (0, 0)))
    response = jnp.zeros((SEQS, LEN, CONV), jnp.float32)
    for tap in range(KERNEL):
        response = response + conv_kernel[tap] * padded[:, tap:tap + LEN]
    conv_out = (exit_rows.astype(jnp.float32) * response.reshape(count, CONV)).astype(jnp.bfloat16)
    concatenated_result = jnp.concatenate([memory_out, conv_out], axis=1)
    mixed = jnp.dot(concatenated_result, merge_weight, preferred_element_type=jnp.float32).astype(jnp.bfloat16)
    return mixed.reshape(SEQS, LEN, D)
```

```python
import jax
import jax.numpy as jnp
from jax import lax
from jax.experimental import pallas as pl
from jax.experimental.pallas import tpu as pltpu
from jax.sharding import PartitionSpec as P

DK = 64
DV = 128
BLOCK = 128
KERNEL = 3


EPSILON = 1e-06
EMPTY_LOG = -1e30
HIGHEST = lax.Precision.HIGHEST


def prefix(part, axis, combine, identity):
    place = lax.axis_index(axis)
    gathered = jax.tree.map(lambda a: lax.all_gather(a, axis), part)
    state = jax.tree.map(lambda a, e: jnp.zeros_like(a) + jnp.asarray(e, a.dtype), part, identity)

    def one(step, state):
        return combine(
            state, jax.tree.map(lambda a: lax.dynamic_index_in_dim(a, step, 0, False), gathered)
        )

    return lax.fori_loop(0, place, one, state)


def passed_along(value, axis, steps):
    count = lax.axis_size(axis)
    initial, last = (max(0, -steps), min(count, count - steps))
    return lax.ppermute(value, axis, [(source, source + steps) for source in range(initial, last)])


def combine(earlier, later):
    ceiling = jnp.maximum(later[2] + earlier[1], later[1])
    kept = jnp.exp(later[2] + earlier[1] - ceiling)
    added = jnp.exp(later[1] - ceiling)
    state = kept[..., None, None] * earlier[0] + added[..., None, None] * later[0]
    return (state, ceiling, earlier[2] + later[2])


def identity_state(heads):
    return (
        jnp.zeros((heads, DK, DV), jnp.float32),
        jnp.full((heads,), EMPTY_LOG, jnp.float32),
        jnp.zeros((heads,), jnp.float32),
    )


def add_product(left, piece):
    return jnp.dot(left, piece, preferred_element_type=jnp.float32)


def split_columns(total, stack):
    outputs = []
    offset = 0
    for weight in stack:
        outputs.append(total[:, offset : offset + weight.shape[1]])
        offset = offset + weight.shape[1]
    return outputs


def incoming_state(running):
    heads = running[1].shape[0]
    before = prefix((running[0], running[1], running[2]), "sp", combine, identity_state(heads))
    ceiling = jnp.maximum(before[1], before[2])
    shrink = jnp.exp(before[1] - ceiling)
    return (before[0] * shrink[:, None, None], ceiling, before[2])


def memory_states(keys, values, gates, forget_bias, forget_shift):
    count = gates.shape[0]
    heads = forget_bias.shape[0]
    blocks = count // BLOCK
    inputs = gates[:, :heads].reshape(blocks, BLOCK, heads)
    logs = jax.nn.log_sigmoid(gates[:, heads:] + forget_bias) + forget_shift[0].T
    cumulative = jnp.cumsum(logs.reshape(blocks, BLOCK, heads), axis=1)
    last = cumulative[:, -1]
    weight_logs = last[:, None, :] - cumulative + inputs
    peak = jnp.max(weight_logs, axis=1)
    coefficient_array = jnp.exp(weight_logs - peak[:, None, :])
    scaled = keys.reshape(blocks, BLOCK, heads, DK).astype(jnp.float32) * DK ** (-0.5)
    value_float = values.reshape(blocks, BLOCK, heads, DV).astype(jnp.float32)
    states = jnp.einsum(
        "csh,cshk,cshv->chkv", coefficient_array, scaled, value_float, precision=HIGHEST
    )
    running = identity_state(heads)
    prefixes = []
    for index in range(blocks):
        prefixes.append(running)
        running = combine(running, (states[index], peak[index], last[index]))
    leading_part = tuple((jnp.stack([item[member] for item in prefixes]) for member in range(3)))
    gate_apertures = combine(incoming_state(running), leading_part)
    return (gate_apertures, cumulative, inputs)


def memory_output(
    queries, keys, values, outgates, inputs, cumulative, gate_apertures, head_norm_gain
):
    blocks = cumulative.shape[0]
    heads = cumulative.shape[2]
    count = queries.shape[0]
    query_blocks = queries.reshape(blocks, BLOCK, heads, DK)
    key_blocks = keys.reshape(blocks, BLOCK, heads, DK)
    value_blocks = values.reshape(blocks, BLOCK, heads, DV)
    score_matrix = jnp.einsum(
        "cjhk,cshk->chjs", query_blocks, key_blocks, preferred_element_type=jnp.float32
    ) * DK ** (-0.5)
    cum_lanes = cumulative.transpose(0, 2, 1)
    input_lanes = inputs.transpose(0, 2, 1)
    causal = jnp.tril(jnp.ones((BLOCK, BLOCK), dtype=bool))
    decay = jnp.where(
        causal,
        cum_lanes[..., :, None] - cum_lanes[..., None, :] + input_lanes[..., None, :],
        -jnp.inf,
    )
    inter = cum_lanes + gate_apertures[1][..., None]
    ceiling = jnp.maximum(inter, jnp.max(decay, axis=-1))
    weighted = score_matrix * jnp.exp(decay - ceiling[..., None])
    numerator = jnp.einsum(
        "chjs,cshv->chjv",
        weighted.astype(jnp.bfloat16),
        value_blocks,
        preferred_element_type=jnp.float32,
    )
    query_float = query_blocks.astype(jnp.float32)
    carried = jnp.exp(inter - ceiling)
    numerator = numerator + carried[..., None] * jnp.einsum(
        "cjhk,chkv->chjv", query_float, gate_apertures[0], precision=HIGHEST
    )
    result = numerator * lax.rsqrt(
        jnp.mean(numerator * numerator, axis=-1, keepdims=True) + EPSILON
    )
    result = result.transpose(0, 2, 1, 3).reshape(count, heads * DV) * head_norm_gain
    return (result * jax.nn.sigmoid(outgates.astype(jnp.float32))).astype(jnp.bfloat16)


def local(
    tokens,
    norm_gain,
    query_weight,
    key_weight,
    value_weight,
    outgate_weight,
    gate_weight,
    forget_bias,
    forget_shift,
    head_norm_gain,
    exit_weight,
    entry_weight,
    signal_weight,
    conv_kernel,
    merge_weight,
):
    whole = lax.all_gather(tokens, "tp", axis=2, tiled=True)[0]
    count = whole.shape[0]
    flat = whole.astype(jnp.float32)
    normed = (
        flat * lax.rsqrt(jnp.mean(flat * flat, axis=-1, keepdims=True) + EPSILON) * norm_gain
    ).astype(jnp.bfloat16)
    gate_rows = gate_weight.reshape(gate_weight.shape[0], -1)
    state_stack = [key_weight, value_weight, gate_rows]
    other_stack = [query_weight, outgate_weight, exit_weight, entry_weight, signal_weight]
    stacked = jnp.concatenate(state_stack + other_stack, axis=1)
    total = add_product(normed, lax.all_gather(stacked, ("sp", "fs"), axis=0, tiled=True))
    columns = split_columns(total, state_stack + other_stack)
    keys = columns[0].astype(jnp.bfloat16)
    values = columns[1].astype(jnp.bfloat16)
    gate_apertures, cumulative, inputs = memory_states(
        keys, values, columns[2], forget_bias, forget_shift
    )
    others = columns[3:]
    queries = others[0].astype(jnp.bfloat16)
    outgates = others[1].astype(jnp.bfloat16)
    exit_rows = others[2].astype(jnp.bfloat16)
    entry_rows = others[3].astype(jnp.bfloat16)
    signal_rows = others[4].astype(jnp.bfloat16)
    mixed_in = (entry_rows.astype(jnp.float32) * signal_rows.astype(jnp.float32)).astype(
        jnp.bfloat16
    )
    rim = passed_along(mixed_in[count - (KERNEL - 1) :], "sp", 1)
    padded = jnp.concatenate([rim, mixed_in], axis=0).astype(jnp.float32)
    response = conv_kernel[0] * padded[0:count]
    for tap in range(1, KERNEL):
        response = response + conv_kernel[tap] * padded[tap : tap + count]
    conv_out = (exit_rows.astype(jnp.float32) * response).astype(jnp.bfloat16)
    memory_out = memory_output(
        queries, keys, values, outgates, inputs, cumulative, gate_apertures, head_norm_gain
    )
    memory_all, conv_all = (
        lax.all_gather(memory_out, "tp", axis=1, tiled=True),
        lax.all_gather(conv_out, "tp", axis=1, tiled=True),
    )
    concatenated_result = jnp.concatenate([memory_all, conv_all], axis=1)
    mixed = add_product(
        concatenated_result, lax.all_gather(merge_weight, ("sp", "fs"), axis=0, tiled=True)
    )
    return mixed.astype(jnp.bfloat16)[None]


MESH = pl.DeviceIdType.MESH


class Place:
    def __init__(self):
        self.z = lax.axis_index("sp")
        f = lax.axis_index("fs")
        self.t = lax.axis_index("tp")
        self.h, self.p = self.z // 2, self.z % 2
        self.y, self.x = f // 2, f % 2
        self.c = self.p * 2 + self.x
        self.xn = {"fs": self.y * 2 + 1 - self.x}
        self.yn = {"fs": (1 - self.y) * 2 + self.x}
        self.tn = {"tp": 1 - self.t}
        self.row = [
            self.z,
            self.h * 2 + 1 - self.p,
            (1 - self.h) * 2 + self.p,
            (1 - self.h) * 2 + 1 - self.p,
        ]
        self.zn = [None] + [{"sp": row} for row in self.row[1:]]
        self.diagonal = {"fs": self.y * 2 + 1 - self.x, "sp": self.row[1]}
        self.block = {
            (i, j): (self.x + i - 2 * i * self.x) * 2 + (self.p + j - 2 * j * self.p)
            for i in range(2)
            for j in range(2)
        }

    def greet(self, peers):
        barrier = pltpu.get_barrier_semaphore()
        for peer in peers:
            pl.semaphore_signal(barrier, inc=1, device_id=peer, device_id_type=MESH)
        pl.semaphore_wait(barrier, len(peers))


class Sender:
    def __init__(self, send_sem, recv_sem):
        self.send_sem, self.recv_sem, self.copies = send_sem, recv_sem, {}

    def make(self, name, source, target, peer):
        index = len(self.copies)
        self.copies[name] = pltpu.make_async_remote_copy(
            src_ref=source,
            dst_ref=target,
            send_sem=self.send_sem.at[index],
            recv_sem=self.recv_sem.at[index],
            device_id=peer,
            device_id_type=MESH,
        )
        return self.copies[name]

    def __call__(self, name, source, target, peer):
        self.make(name, source, target, peer).start()

    def arrived(self, name):
        self.copies[name].wait_recv()

    def drain(self):
        for copy in self.copies.values():
            copy.wait_send()


MERGE_SLICES = 2


def layer_kernel(heads, groups, *refs):
    widths = sum(groups, [])
    count = len(widths)
    gain_ref, tokens_ref, shift_ref, gate_ref, bias_ref, head_gain_ref, taps_ref, merge_ref = refs[:8]
    weights = refs[8 : 8 + count]
    out_ref = refs[8 + count]
    (
        tok,
        normed,
        stage,
        transit,
        rows_ref,
        gate_rows,
        shifts_ref,
        proj,
        parts,
        pieces,
        both,
        entered,
        held,
        keys_t,
        u_ref,
        top_ref,
        last_ref,
        states,
        stable,
        decayed,
        final_state,
        final_log,
        came_state,
        came_log,
        rim,
        came_rim,
        own_sum,
        partial,
        came,
        relayed,
        local,
        send_sem,
        recv_sem,
    ) = refs[9 + count :]
    at = Place()
    z, y, x, t, p, c = at.z, at.y, at.x, at.t, at.p, at.c
    mine, by_z, by_x, by_both = (at.block[i] for i in ((0, 0), (0, 1), (1, 0), (1, 1)))
    depth = weights[0].shape[0]
    half_rows = parts.shape[1]
    broad = rows_ref.shape[2]
    tokens = tok.shape[2]
    features = normed.shape[1]
    width_t = features // 2
    per = tokens // BLOCK
    blocks = 2 * per
    other_x, other_p = 1 - x, 1 - p
    kept = []

    def fetch(source, target):
        copy = pltpu.make_async_copy(source, target, local.at[len(kept)])
        copy.start()
        kept.append(copy)

    def rows_of(k, beside, side):
        row = at.row[k] * 4 + (1 - y if beside else y) * 2 + (other_x if side else x)
        return pl.ds(pl.multiple_of(row * depth, depth), depth)

    def slab(k, side, s):
        return rows_ref.at[s, rows_of(k, False, side)]

    def lanes(k, side):
        return gate_rows.at[:, rows_of(k, False, side)]

    fetch(tokens_ref, tok.at[mine, t])
    fetch(shift_ref, shifts_ref.at[mine])
    fetch(gate_ref, lanes(0, 0))
    fetch(merge_ref.at[pl.ds(0, half_rows)], parts.at[y])
    for quarter in range(4):
        index = 0
        for s, group in enumerate(groups):
            offset = 0
            for width in group:
                fetch(
                    weights[index].at[:, pl.ds(quarter * width, width)],
                    stage.at[quarter, s, :, pl.ds(offset, width)],
                )
                offset += width
                index += 1
    at.greet([at.xn, at.yn, at.tn, at.diagonal] + at.zn[1:])
    for copy in kept:
        copy.wait()

    send = Sender(send_sem, recv_sem)

    def to_z(side, s):
        for k in (1, 3, 2):
            if side:
                source = slab(0, 1, s) if k == 2 else transit.at[s]
            else:
                source = stage.at[(p if k == 2 else other_p) * 2 + x, s]
            send(("z", k, side, s), source, slab(0, side, s), at.zn[k])

    for k in (1, 2, 3):
        send(("zg", k, 0), lanes(0, 0), lanes(0, 0), at.zn[k])
    send("x gate", lanes(0, 0), lanes(0, 0), at.xn)
    send(("yg", 0, 0), lanes(0, 0), lanes(0, 0), at.yn)
    send("x shift", shifts_ref.at[mine], shifts_ref.at[mine], at.xn)
    send("z shift", shifts_ref.at[mine], shifts_ref.at[mine], at.zn[1])

    def to_x(s):
        send(("x same", s), stage.at[p * 2 + other_x, s], slab(0, 0, s), at.xn)
        send(("x other", s), stage.at[other_p * 2 + other_x, s], transit.at[s], at.xn)

    def to_y(side, s):
        source = slab(0, 1, s) if side else stage.at[c, s]
        send(("y", 0, side, s), source, slab(0, side, s), at.yn)

    to_x(0)
    to_z(0, 0)
    to_y(0, 0)
    send("t own", tok.at[mine, t], tok.at[mine, t], at.tn)
    send("z tok", tok.at[mine, t], tok.at[mine, t], at.zn[1])
    send("part", merge_ref.at[pl.ds(half_rows, half_rows)], parts.at[y], at.yn)
    for s in range(len(groups)):
        rows_ref[s, rows_of(0, False, 0), :] = stage[c, s]

    gain = gain_ref[...]
    step = 16

    def normalize(block):
        def one(i, carry):
            local_rows = pl.ds(pl.multiple_of(i * step, step), step)
            halves = [tok[block, side, local_rows, :].astype(jnp.float32) for side in range(2)]
            total = sum(jnp.sum(a * a, axis=1, keepdims=True) for a in halves)
            scale = lax.rsqrt(total / features + EPSILON)
            place = pl.ds(pl.multiple_of(block * tokens + i * step, step), step)
            for side in range(2):
                columns = slice(side * width_t, (side + 1) * width_t)
                value = halves[side] * scale * gain[:, columns]
                normed[place, columns] = value.astype(jnp.bfloat16)
            return carry

        lax.fori_loop(0, tokens // step, one, 0, unroll=4)

    def project(block, s):
        place = pl.ds(pl.multiple_of(block * tokens, tokens), tokens)

        def one(n, carry):
            columns = pl.ds(pl.multiple_of(n * 512, 512), 512)
            product = jnp.dot(
                normed[place, :], rows_ref[s, :, columns], preferred_element_type=jnp.float32
            )
            proj[s, place, columns] = product.astype(jnp.bfloat16)
            return carry

        lax.fori_loop(0, broad // 512, one, 0)

    def forward(side, s):
        for k in (1, 3, 2):
            if s == 0:
                send.arrived(("zg", k, side))
                send(("yg", k, side), lanes(k, side), lanes(k, side), at.yn)
            send.arrived(("z", k, side, s))
            send(("y", k, side, s), slab(k, side, s), slab(k, side, s), at.yn)

    def all_here(s):
        for k in range(4):
            for side in range(2):
                send.arrived(("y", k, side, s))

    half_at = (y + p - 2 * y * p) * half_rows
    out_strip = pieces.shape[2] // MERGE_SLICES

    def merge_half(k, parity, s):
        side = y + parity - 2 * y * parity
        place = pl.ds(pl.multiple_of(side * half_rows, half_rows), half_rows)
        return pieces.at[at.row[k], place, pl.ds(s * out_strip, out_strip)]

    def merge_to_z(s):
        for k in (1, 3, 2):
            source = parts.at[p if k == 2 else other_p, :, pl.ds(s * out_strip, out_strip)]
            parity = p if k == 2 else other_p
            send(("m", k, s), source, merge_half(0, parity, s), at.zn[k])

    def merge_to_y(s):
        source = parts.at[p, :, pl.ds(s * out_strip, out_strip)]
        send(("my", 0, s), source, merge_half(0, p, s), at.yn)

    def forward_merge(s):
        for k in (1, 3, 2):
            send.arrived(("m", k, s))
            send(("my", k, s), merge_half(k, p, s), merge_half(k, p, s), at.yn)

    send.arrived("t own")
    normalize(mine)
    send.arrived(("x same", 0))
    to_y(1, 0)
    send.arrived("x gate")
    send(("yg", 0, 1), lanes(0, 1), lanes(0, 1), at.yn)
    for k in (1, 2, 3):
        send(("zg", k, 1), lanes(0, 1), lanes(0, 1), at.zn[k])
    send.arrived(("x other", 0))
    to_z(1, 0)
    send("x tok", tok.at[mine, t], tok.at[mine, t], at.xn)
    to_x(1)
    to_z(0, 1)
    forward(0, 0)
    to_z(0, 2)
    to_y(0, 1)
    send.arrived("part")
    pieces[z, pl.ds(pl.multiple_of(half_at, half_rows), half_rows), :] = parts[p]
    forward(1, 0)
    to_y(0, 2)
    send.arrived("z tok")
    send("t z", tok.at[by_z, t], tok.at[by_z, t], at.tn)
    send.arrived("z shift")
    send.arrived("x tok")
    send("t x", tok.at[by_x, t], tok.at[by_x, t], at.tn)
    to_x(2)
    send("x tok on", tok.at[by_z, t], tok.at[by_z, t], at.xn)
    send("x shift on", shifts_ref.at[by_z], shifts_ref.at[by_z], at.xn)
    send.arrived(("x same", 1))
    to_y(1, 1)
    send.arrived(("x other", 1))
    to_z(1, 1)
    send.arrived("t z")
    normalize(by_z)
    forward(0, 1)
    send.arrived("t x")
    normalize(by_x)
    for k in range(4):
        for side in range(2):
            send.arrived(("yg", k, side))
    all_here(0)

    kq, kv = heads * DK, heads * DV
    q_at, k_at, v_at = 0, groups[0][0], groups[0][0] + groups[0][1]
    conv = groups[1][0]
    scale = DK ** (-0.5)
    lane = lax.broadcasted_iota(jnp.int32, (BLOCK, BLOCK), 1)
    sub = lax.broadcasted_iota(jnp.int32, (BLOCK, BLOCK), 0)
    causal = lane <= sub
    upto = (sub <= lane).astype(jnp.float32)
    which = lax.broadcasted_iota(jnp.int32, shifts_ref.shape[1:], 0)
    tp_heads = gate_rows.shape[0] // 2

    def by_block(line):
        return jnp.concatenate(
            [line[:, i * BLOCK : (i + 1) * BLOCK] for i in range(blocks)], axis=0
        )

    def pick(array, index):
        line = lax.broadcasted_iota(jnp.int32, array.shape, 0)
        return jnp.sum(jnp.where(index == line, array, 0.0), axis=0, keepdims=True)

    def block_rows(r):
        return pl.ds(pl.multiple_of(r * BLOCK, BLOCK), BLOCK)

    def recur(q):
        place = pl.ds(pl.multiple_of(q * 2 * tokens, 2 * tokens), 2 * tokens)
        gates = lax.dot_general(
            gate_rows[...],
            normed[place, :],
            (((1,), (1,)), ((), ())),
            preferred_element_type=jnp.float32,
        )
        for hh in range(heads):
            head = c * heads + hh
            entry = by_block(pick(gates, head))
            forget = by_block(pick(gates, tp_heads + head)) + bias_ref[head]
            shift = by_block(
                jnp.concatenate([pick(shifts_ref[q * 2 + j], head) for j in range(2)], axis=1)
            )
            logs = jnp.minimum(forget, 0.0) - jnp.log1p(jnp.exp(-jnp.abs(forget))) + shift
            cumulative = jnp.dot(
                logs, upto, precision=HIGHEST, preferred_element_type=jnp.float32
            )
            u = entry - cumulative
            top = jnp.broadcast_to(jnp.max(u, axis=1, keepdims=True), u.shape)
            last = jnp.broadcast_to(cumulative[:, BLOCK - 1 :], u.shape)
            for i in range(blocks):
                u_ref[hh, q * blocks + i] = u[i : i + 1]
                top_ref[hh, q * blocks + i] = top[i : i + 1]
                last_ref[hh, q * blocks + i] = last[i : i + 1]
        for hh in range(heads):
            final_state[q, hh] = jnp.zeros((DK, DV), jnp.float32)

        def scan(i, carry):
            r = q * blocks + i
            keys = proj[0, block_rows(r), k_at : k_at + kq].astype(jnp.float32).T
            keys_t[r] = keys.astype(jnp.bfloat16)
            out = []
            for hh, (m, total) in enumerate(carry):
                last = last_ref[hh, r]
                state = final_state[q, hh]
                states[hh, r] = state
                stable[hh, r] = m
                decayed[hh, r] = total
                peak = jnp.maximum(m, top_ref[hh, r])
                weight = jnp.exp(u_ref[hh, r] - peak) * scale
                weighted = (keys[hh * DK : (hh + 1) * DK] * weight).astype(jnp.bfloat16)
                values = proj[0, block_rows(r), v_at + hh * DV : v_at + (hh + 1) * DV]
                final_state[q, hh] = jnp.exp(m - peak) * state + jnp.dot(
                    weighted, values, preferred_element_type=jnp.float32
                )
                out.append((last + peak, total + last))
            return tuple(out)

        start = tuple(
            (jnp.full((1, BLOCK), EMPTY_LOG, jnp.float32), jnp.zeros((1, BLOCK), jnp.float32))
            for _ in range(heads)
        )
        ended = lax.fori_loop(0, blocks, scan, start)
        for hh, (m, total) in enumerate(ended):
            peak = jnp.maximum(m, total)
            final_state[q, hh] = jnp.exp(m - peak) * final_state[q, hh]
            final_log[q, hh : hh + 1, :] = peak
        send(("state", len(send.copies)), final_state.at[q], came_state.at[q], at.zn[2])
        send(("log", len(send.copies)), final_log.at[q], came_log.at[q], at.zn[2])
        return list(send.copies)[-2:]

    later = at.h == 1
    head_gain = head_gain_ref[:, pl.ds(pl.multiple_of(c * kv, kv), kv)]
    nothing = jnp.zeros((DK, BLOCK), jnp.bfloat16)

    def only(hh, value):
        return jnp.concatenate([value if h == hh else nothing for h in range(heads)], axis=0)

    def cell(b, q):
        def one(i, carry):
            r = b * per + i
            queries = proj[0, block_rows(r), q_at : q_at + kq]
            right, carried = [], []
            for hh in range(heads):
                right.append(only(hh, keys_t[r, hh * DK : (hh + 1) * DK, :]))
            for hh in range(heads):
                m = stable[hh, r]
                m_in = decayed[hh, r] + jnp.where(later, came_log[q, hh : hh + 1, :], 0.0)
                peak = jnp.maximum(m, m_in)
                state = jnp.exp(m - peak) * states[hh, r] + jnp.exp(m_in - peak) * jnp.where(
                    later, came_state[q, hh], 0.0
                )
                right.append(only(hh, state.astype(jnp.bfloat16)))
                carried.append(peak)
            product = jnp.dot(
                queries, jnp.concatenate(right, axis=1), preferred_element_type=jnp.float32
            )
            for hh in range(heads):
                u = jnp.where(causal, u_ref[hh, r], EMPTY_LOG)
                peak = jnp.maximum(jnp.max(u, axis=1, keepdims=True), carried[hh])
                weighted = product[:, hh * BLOCK : (hh + 1) * BLOCK] * scale * jnp.exp(u - peak)
                values = proj[0, block_rows(r), v_at + hh * DV : v_at + (hh + 1) * DV]
                numerator = jnp.dot(
                    weighted.astype(jnp.bfloat16), values, preferred_element_type=jnp.float32
                )
                inter = product[:, heads * BLOCK + hh * DV : heads * BLOCK + (hh + 1) * DV]
                numerator = numerator + jnp.exp(carried[hh] - peak) * inter
                mean = jnp.mean(numerator * numerator, axis=1, keepdims=True)
                lanes_h = slice(hh * DV, (hh + 1) * DV)
                held[block_rows(r), lanes_h] = (
                    numerator * lax.rsqrt(mean + EPSILON) * head_gain[:, lanes_h]
                )
            return carry

        lax.fori_loop(0, per, one, 0)

    edge = entered.shape[1] - blocks * BLOCK

    def enter(q):
        def one(i, carry):
            rows = block_rows(q * blocks + i)
            value = proj[1, rows, 0:conv].astype(jnp.float32) * proj[
                1, rows, conv : 2 * conv
            ].astype(jnp.float32)
            value = value.astype(jnp.bfloat16).astype(jnp.float32)
            entered[q, pl.ds(pl.multiple_of(edge + i * BLOCK, edge), BLOCK), :] = value
            return carry

        lax.fori_loop(0, blocks, one, 0)
        rim[q] = entered[q, blocks * BLOCK : blocks * BLOCK + edge, :].astype(jnp.bfloat16)

    def respond():
        taps = taps_ref[:, pl.ds(pl.multiple_of(c * conv, conv), conv)]
        for q in range(2):
            before = came_rim[q].astype(jnp.float32)
            entered[q, 0:edge, :] = jnp.where(later, before, 0.0)
            for i in range(blocks):
                first = edge + i * BLOCK - (KERNEL - 1)
                response = taps[0:1] * entered[q, first : first + BLOCK, :]
                for tap in range(1, KERNEL):
                    response = response + taps[tap : tap + 1] * entered[
                        q, first + tap : first + tap + BLOCK, :
                    ]
                start = (q * blocks + i) * BLOCK
                held[start : start + BLOCK, kv : kv + conv] = response

    def close(b):
        project(b, 2)

        def one(i, carry):
            rows = block_rows(b * per + i)
            opened = jax.nn.sigmoid(proj[2, rows, 0:kv].astype(jnp.float32))
            both[t, b, block_rows(i), 0:kv] = (held[rows, 0:kv] * opened).astype(jnp.bfloat16)
            value = proj[2, rows, kv : kv + conv].astype(jnp.float32) * held[rows, kv : kv + conv]
            both[t, b, block_rows(i), kv : kv + conv] = value.astype(jnp.bfloat16)
            return carry

        lax.fori_loop(0, per, one, 0)

    for b in (mine, by_z):
        project(b, 0)
    send.arrived(("x same", 2))
    to_y(1, 2)
    send.arrived(("x other", 2))
    to_z(1, 2)
    forward(0, 2)
    came_own = recur(x)
    project(by_x, 0)
    forward(1, 1)
    merge_to_z(0)
    merge_to_y(0)
    for name in came_own:
        send.arrived(name)
    cell(mine, x)
    cell(by_z, x)
    send.arrived("x tok on")
    send("t zx", tok.at[by_both, t], tok.at[by_both, t], at.tn)
    send.arrived("x shift")
    send.arrived("x shift on")
    forward(1, 2)
    for s in range(1, MERGE_SLICES):
        merge_to_z(s)
        merge_to_y(s)
    send.arrived("t zx")
    normalize(by_both)
    project(by_both, 0)
    came_other = recur(other_x)
    all_here(1)
    for b in (mine, by_z):
        project(b, 1)
    forward_merge(0)
    for b in (by_x, by_both):
        project(b, 1)
    for q in range(2):
        enter(q)
    send("rim", rim, came_rim, at.zn[2])
    for name in came_other:
        send.arrived(name)
    for s in range(1, MERGE_SLICES):
        forward_merge(s)
    cell(by_both, other_x)
    cell(by_x, other_x)
    send.arrived("rim")
    respond()
    all_here(2)

    columns = out_ref.shape[1]
    rows_half = tokens // 2

    def merge(b, part, s):
        rows = pl.ds(part * rows_half, rows_half)
        place = pl.ds(s * out_strip, out_strip)
        total = None
        for side in range(2):
            for group, (start, width) in enumerate(((0, kv), (kv, conv))):
                product = jnp.dot(
                    both[side, b, rows, start : start + width],
                    pieces[group * 2 + side, :, place],
                    preferred_element_type=jnp.float32,
                )
                total = product if total is None else total + product
        return total

    def pass_on(name, s, index, b, part, peer, extra=None):
        rows = pl.ds(part * rows_half, rows_half)
        place = pl.ds(s * out_strip, out_strip)
        total = merge(b, part, s)
        if extra is not None:
            total = total + relayed[extra, :, place].astype(jnp.float32)
        partial[index, rows, place] = total.astype(jnp.bfloat16)
        target = relayed.at[part, :, place] if index == 2 else came.at[index, rows, place]
        send((name, s), partial.at[index, rows, place], target, peer)

    def swap(step, b):
        close(b)
        send(("t", step), both.at[t, b], both.at[t, b], at.tn)

    for step, b in enumerate((by_both, by_x, by_z, mine)):
        swap(step, b)
    for s in range(MERGE_SLICES):
        for k in range(4):
            send.arrived(("my", k, s))
        for step in range(3 if s == 0 else 0):
            send.arrived(("t", step))
        pass_on("sum d0", s, 2, by_both, 0, at.xn)
        pass_on("sum d1", s, 2, by_both, 1, at.zn[1])
        pass_on("sum x0", s, 0, by_x, 0, at.xn)
        pass_on("sum z1", s, 1, by_z, 1, at.zn[1])
    send.arrived(("t", 3))
    for s in range(MERGE_SLICES):
        send.arrived(("sum d0", s))
        pass_on("sum z0", s, 1, by_z, 0, at.zn[1], 0)
        send.arrived(("sum d1", s))
        pass_on("sum x1", s, 0, by_x, 1, at.xn, 1)
        for part in range(2):
            place = pl.ds(s * out_strip, out_strip)
            own_sum[pl.ds(part * rows_half, rows_half), place] = merge(mine, part, s)
    for s in range(MERGE_SLICES):
        for part, names in ((0, ("sum x0", "sum z0")), (1, ("sum z1", "sum x1"))):
            for name in names:
                send.arrived((name, s))
            rows = slice(part * rows_half, (part + 1) * rows_half)
            place = slice(s * out_strip, (s + 1) * out_strip)
            total = own_sum[rows, place] + came[0, rows, place].astype(jnp.float32)
            total = total + came[1, rows, place].astype(jnp.float32)
            out_ref[rows, place] = total.astype(jnp.bfloat16)
    send.drain()


def layer(gain, tokens, shift, gate_rows, bias, head_gain, taps, merge, heads, grouped):
    weights = sum(grouped, [])
    rows, width_t = tokens.shape
    columns = merge.shape[1]
    features = 2 * width_t
    depth = weights[0].shape[0]
    groups = [[w.shape[1] // 4 for w in group] for group in grouped]
    broad = sum(groups[0])
    gates = gate_rows.shape[0]
    kv, conv, m_depth = heads * DV, groups[1][0], merge.shape[0]
    blocks = 4 * rows // BLOCK
    vmem = pl.BlockSpec(memory_space=pltpu.VMEM)
    hbm = pl.BlockSpec(memory_space=pl.ANY)
    smem = pl.BlockSpec(memory_space=pltpu.SMEM)
    f32, bf16 = jnp.float32, jnp.bfloat16
    return pl.pallas_call(
        lambda *refs: layer_kernel(heads, groups, *refs),
        out_shape=jax.ShapeDtypeStruct((rows, columns), bf16),
        in_specs=[vmem, hbm, hbm, hbm, smem, vmem, vmem, hbm] + [hbm] * len(weights),
        out_specs=vmem,
        scratch_shapes=[
            pltpu.VMEM((4, 2, rows, width_t), bf16),
            pltpu.VMEM((4 * rows, features), bf16),
            pltpu.VMEM((4, len(groups), depth, broad), bf16),
            pltpu.VMEM((len(groups), depth, broad), bf16),
            pltpu.VMEM((len(groups), features, broad), bf16),
            pltpu.VMEM((gates, features), bf16),
            pltpu.VMEM((4,) + shift.shape, f32),
            pltpu.VMEM((len(groups), 4 * rows, broad), bf16),
            pltpu.VMEM((2, m_depth // 2, columns), bf16),
            pltpu.VMEM((4, m_depth, columns), bf16),
            pltpu.VMEM((2, 4, rows, kv + conv), bf16),
            pltpu.VMEM((2, 16 + 2 * rows, conv), f32),
            pltpu.VMEM((4 * rows, kv + conv), f32),
            pltpu.VMEM((blocks, heads * DK, BLOCK), bf16),
            pltpu.VMEM((heads, blocks, 1, BLOCK), f32),
            pltpu.VMEM((heads, blocks, 1, BLOCK), f32),
            pltpu.VMEM((heads, blocks, 1, BLOCK), f32),
            pltpu.VMEM((heads, blocks, DK, DV), f32),
            pltpu.VMEM((heads, blocks, 1, BLOCK), f32),
            pltpu.VMEM((heads, blocks, 1, BLOCK), f32),
            pltpu.VMEM((2, heads, DK, DV), f32),
            pltpu.VMEM((2, heads, BLOCK), f32),
            pltpu.VMEM((2, heads, DK, DV), f32),
            pltpu.VMEM((2, heads, BLOCK), f32),
            pltpu.VMEM((2, 16, conv), bf16),
            pltpu.VMEM((2, 16, conv), bf16),
            pltpu.VMEM((rows, columns), f32),
            pltpu.VMEM((3, rows, columns), bf16),
            pltpu.VMEM((2, rows, columns), bf16),
            pltpu.VMEM((2, rows // 2, columns), bf16),
            pltpu.SemaphoreType.DMA((4 + 4 * len(weights),)),
            pltpu.SemaphoreType.DMA((112,)),
            pltpu.SemaphoreType.DMA((112,)),
        ],
        compiler_params=pltpu.CompilerParams(
            collective_id=0, has_side_effects=True, vmem_limit_bytes=67043328
        ),
        cost_estimate=pl.CostEstimate(
            flops=8 * rows * features * broad * len(groups), bytes_accessed=0, transcendentals=0
        ),
        name="layer",
    )(gain, tokens, shift, gate_rows, bias, head_gain, taps, merge, *weights)


def regrouped(
    tokens,
    norm_gain,
    query_weight,
    key_weight,
    value_weight,
    outgate_weight,
    gate_weight,
    forget_bias,
    forget_shift,
    head_norm_gain,
    exit_weight,
    entry_weight,
    signal_weight,
    conv_kernel,
    merge_weight,
):
    grouped = [
        [query_weight, key_weight, value_weight],
        [entry_weight, signal_weight],
        [outgate_weight, exit_weight],
    ]
    heads = gate_weight.shape[2] // 4
    gate_rows = gate_weight.reshape(gate_weight.shape[0], -1).T
    mixed = layer(
        norm_gain[None],
        tokens[0],
        forget_shift[0],
        gate_rows,
        forget_bias,
        head_norm_gain[None],
        conv_kernel,
        merge_weight,
        heads,
        grouped,
    )
    return mixed[None]


def solution(mesh):
    placed = (
        P("fs", "sp", "tp"),
        P(),
        P(("sp", "fs"), "tp"),
        P(("sp", "fs"), "tp"),
        P(("sp", "fs"), "tp"),
        P(("sp", "fs"), "tp"),
        P(("sp", "fs"), None, "tp"),
        P("tp"),
        P("fs", "tp", "sp"),
        P("tp"),
        P(("sp", "fs"), "tp"),
        P(("sp", "fs"), "tp"),
        P(("sp", "fs"), "tp"),
        P(None, "tp"),
        P(("sp", "fs"), "tp"),
    )
    sp, tp = mesh.shape["sp"], mesh.shape["tp"]

    def step(*args):
        square = (sp, mesh.shape["fs"], tp) == (4, 4, 2)
        body = regrouped if square else local
        return jax.shard_map(
            body, mesh=mesh, in_specs=placed, out_specs=P("fs", "sp", "tp"), check_vma=False
        )(*args)

    return step
```
